32 devices in a mesh: ep: 8 (over z, y), tp: 4 (over x, core).
Axes of the slice: x: 2, y: 2, z: 4, core: 2. Of those that a mesh axis runs over, the one named last changes fastest.
Arguments:
- queries_a: bfloat16 [1024, 1024], P('ep', 'tp'), may hold values from -128 to 128
- queries_b: bfloat16 [1024, 1024], P('ep', 'tp'), may hold values from -128 to 128
- keys_a: bfloat16 [1024, 512], P('ep', 'tp'), may hold values from -8 to 8
- keys_b: bfloat16 [1024, 512], P('ep', 'tp'), may hold values from -8 to 8
- values: bfloat16 [1024, 1024], P('ep', 'tp'), may hold values from -6 to 6
- lambdas: float32 [16], P('tp'), may hold values from 0.3 to 0.8
- head_gain: float32 [128], replicated, may hold values from 0.1 to 1.9
- w_out: bfloat16 [2048, 2048], P('tp'), may hold values from -0.125 to 0.125
- moe_tokens: bfloat16 [4096, 2048], P(('ep', 'tp')), may hold values from -80 to 80
- moe_gain: float32 [2048], replicated, may hold values from 0.1 to 1.9
- routes: int32 [4096, 2], P(('ep', 'tp')), may hold values from 0 to 7, all different within a row; in each aligned block of 128 rows (0 to 127, 128 to 255, ...) at most 48 rows name the same one
- route_weights: float32 [4096, 2], P(('ep', 'tp')), may hold values from 0.1 to 1
- w_gate: bfloat16 [8, 2048, 2048], P('ep', None, 'tp'), may hold values from -4 to 4
- w_up: bfloat16 [8, 2048, 2048], P('ep', None, 'tp'), may hold values from -4 to 4
- w_down: bfloat16 [8, 2048, 2048], P('ep', 'tp'), may hold values from -0.0625 to 0.0625
Outputs:
- mixer_out: bfloat16 [1024, 2048], P(('ep', 'tp'))
- moe_out: bfloat16 [4096, 2048], P(('ep', 'tp'))
The draws below stay inside these ranges and needn't reach their ends.
Inputs may be any that keep to these rules, and one draw needn't show every extreme that they name: `routes`: each row names 2 different experts. Within the rows of one device no expert is named by more than 48 rows, a bound that some block reaches of some device.
All inputs are finite; a program needn't handle non-finite values.
Results may differ from the reference program's by a relative error of at most 0.011.
Values may be sent and summed in bfloat16 or wider, within the bound.
A program may use at most 192 MiB of HBM per device.

```python
import math
import jax
import jax.numpy as jnp
import numpy as np
from jax import lax

D = 2048
HEADS = 16
KV_HEADS = 8
HEAD = 64
VDIM = 128
FF = 2048
TOP = 2
ATT_DEV = 128
TOKB = 128
EXPERTS = 8
CAP = 48
SEQ = 1024
MOE_TOK = 4096
N_EP = 8
N_TP = 4


def query_key_pair(key, which):
    streams = jax.random.split(jax.random.fold_in(key, 1000 + which), 2)
    queries = 1.3 * jnp.clip(jax.random.normal(streams[0], (SEQ, HEADS * HEAD), jnp.float32), -4.0, 4.0)
    keys = 1.3 * jnp.clip(jax.random.normal(streams[1], (SEQ, KV_HEADS * HEAD), jnp.float32), -4.0, 4.0)
    return (queries, keys)


def draw_queries_a(key, part):
    return query_key_pair(key, 0)[0].astype(jnp.bfloat16)


def draw_keys_a(key, part):
    return query_key_pair(key, 0)[1].astype(jnp.bfloat16)


def draw_queries_b(key, part):
    return query_key_pair(key, 1)[0].astype(jnp.bfloat16)


def draw_keys_b(key, part):
    return query_key_pair(key, 1)[1].astype(jnp.bfloat16)


def draw_moe_tokens(key, part):
    streams = jax.random.split(jax.random.fold_in(key, 2000), 3)
    base = jnp.clip(jax.random.normal(streams[0], (MOE_TOK, D), jnp.float32), -4.0, 4.0)
    row_scale = jnp.exp(jax.random.uniform(streams[1], (MOE_TOK, 1), jnp.float32, math.log(0.3), math.log(3.0)))
    column_scale = jnp.exp(jax.random.uniform(streams[2], (1, D), jnp.float32, math.log(0.3), math.log(3.0)))
    result = base * row_scale * column_scale
    return result.astype(jnp.bfloat16)


def expert_matrix(key, salt):
    streams = jax.random.split(jax.random.fold_in(key, salt), 2)
    base = jnp.clip(jax.random.normal(streams[0], (EXPERTS, D, FF), jnp.float32), -4.0, 4.0) / math.sqrt(D)
    spread = jax.random.uniform(streams[1], (EXPERTS, 1, FF), jnp.float32, math.log(0.3), math.log(4.0))
    return (base * jnp.exp(spread)).astype(jnp.bfloat16)


def draw_w_gate(key, part):
    return expert_matrix(key, 3000)


def draw_w_up(key, part):
    return expert_matrix(key, 4000)


def block_scale(stream_key, extent, cuts, least, high):
    gain, own = 1.0, jax.random.fold_in(stream_key, 6)
    for position, parts in cuts:
        heights = jnp.exp(jax.random.uniform(jax.random.fold_in(own, position), (parts,), jnp.float32, least / len(cuts), high / len(cuts)))
        gain = gain * jnp.repeat(heights, extent[position] // parts).reshape([-1 if axis == position else 1 for axis in range(len(extent))])
    return gain


def deal_out(stream_key, own, number, rows, number_of, top, limit, skew):
    sequence = jax.random.permutation(stream_key, number_of)
    heavy_load, ordinary = shares(number_of, rows * top, limit, skew, True), shares(number_of, rows * top, limit, skew, False)
    places = jnp.arange(number_of)

    def named(tallies, offset_by):
        used = int((tallies > 0).sum())
        fixed = max(1, used // 4)
        shifted = fixed + (places - fixed + offset_by * (used - fixed)) % max(1, number_of - fixed)
        return jnp.zeros((number_of,), jnp.int32).at[sequence[jnp.where(places < fixed, places, shifted)]].set(jnp.asarray(tallies, jnp.int32))

    tallies = jnp.where(number % 4 == 0, named(heavy_load, number // 4), named(ordinary, number - number // 4 - 1))
    mixed = jax.random.permutation(jax.random.fold_in(own, 3), number_of)
    source_of, taker = mixed[0:number_of // 2 * 2:2], mixed[1:number_of // 2 * 2:2]
    slack = jnp.minimum(tallies[source_of] - 1, limit - tallies[taker]) // 2
    slack = jnp.where((source_of == sequence[0]) | (taker == sequence[0]) | (tallies[taker] == 0), 0, jnp.maximum(slack, 0))
    shifted = jax.random.randint(jax.random.fold_in(own, 4), (number_of // 2,), 0, 1 << 20) % (slack + 1)
    tallies = tallies.at[source_of].add(-shifted).at[taker].add(shifted)
    items = jnp.searchsorted(jnp.cumsum(tallies), jnp.arange(rows * top), side="right").astype(jnp.int32)
    grid = items.reshape(top, rows).T
    grid = grid[jax.random.permutation(jax.random.fold_in(own, 1), rows)]
    offset_by = jax.random.randint(jax.random.fold_in(own, 2), (rows, 1), 0, top)
    return jnp.take_along_axis(grid, (jnp.arange(top)[None, :] + offset_by) % top, axis=1)


def shares(number_of, total, most, slope, full):
    weights = [(1 << 20) // math.isqrt(rank ** slope) + 1 for rank in range(1, number_of + 1)]
    largest = most if full else min(most, max(-(-total // number_of), total * weights[0] // sum(weights)))
    least = 1 if total - largest >= number_of - 1 else 0
    given, rest = [largest] + [least] * (number_of - 1), total - largest - least * (number_of - 1)
    while rest > 0:
        free = [i for i in range(1, number_of) if given[i] < largest] or [i for i in range(1, number_of) if given[i] < most]
        whole, remaining = sum([weights[i] for i in free]), rest
        for i in free:
            addition = min(most - given[i], max(1, remaining * weights[i] // whole), rest)
            given[i] = given[i] + addition
            rest = rest - addition
    return np.array(given)


def bell_draw(key, shape, deviation, limit, shards=(), held_as=jnp.bfloat16):
    drawn = deviation * jax.random.normal(key, shape, jnp.float32)
    if shards:
        drawn = drawn * block_scale(key, shape, shards, -0.22, 0.18)
    return jnp.clip(drawn, -limit, limit).astype(held_as)


def setup_inputs(seed: int = 0) -> dict:
    key_list = jax.random.split(jax.random.key(seed), 16)
    queries_a = draw_queries_a(jax.random.fold_in(key_list[15], 71), 0)
    queries_b = draw_queries_b(jax.random.fold_in(key_list[15], 71), 0)
    keys_a = draw_keys_a(jax.random.fold_in(key_list[15], 71), 0)
    keys_b = draw_keys_b(jax.random.fold_in(key_list[15], 71), 0)
    values = bell_draw(key_list[4], (SEQ, KV_HEADS * VDIM), 1.0, 6.0, ((0, 8), (1, 4)))
    lambdas = jnp.clip(0.3 + 0.5 * jax.random.uniform(key_list[5], (HEADS,), jnp.float32) ** block_scale(key_list[5], (HEADS,), ((0, 4),), -0.2, 0.2), 0.3, 0.8)
    head_gain = jnp.clip(1.0 + 0.18 * jax.random.normal(key_list[6], (VDIM,), jnp.float32), 0.1, 1.9)
    w_out = bell_draw(key_list[7], (HEADS * VDIM, D), (HEADS * VDIM) ** -0.5, 0.125, ((0, 4),))
    moe_tokens = draw_moe_tokens(jax.random.fold_in(key_list[15], 71), 0)
    moe_gain = jnp.clip(1.0 + 0.18 * jax.random.normal(key_list[9], (D,), jnp.float32), 0.1, 1.9)
    routes_keys = jax.random.split(jax.random.fold_in(key_list[10], 1), MOE_TOK // TOKB)
    routes_turns = jax.random.permutation(jax.random.fold_in(key_list[10], 3), MOE_TOK // TOKB)
    routes = jax.vmap(lambda own, number: deal_out(jax.random.fold_in(key_list[10], 2), own, number, TOKB, EXPERTS, TOP, CAP, 2))(routes_keys, routes_turns).reshape((MOE_TOK, TOP))
    route_weights = jnp.clip(0.1 + 0.9 * jax.random.uniform(key_list[11], (MOE_TOK, TOP), jnp.float32) ** block_scale(key_list[11], (MOE_TOK, TOP), ((0, 32),), -0.2, 0.2), 0.1, 1.0)
    w_gate = draw_w_gate(jax.random.fold_in(key_list[15], 71), 0)
    w_up = draw_w_up(jax.random.fold_in(key_list[15], 71), 0)
    w_down = bell_draw(key_list[14], (EXPERTS, FF, D), (4 * FF) ** -0.5, 0.0625, ((0, 8), (1, 4)))
    return {"queries_a": queries_a, "queries_b": queries_b, "keys_a": keys_a, "keys_b": keys_b, "values": values, "lambdas": lambdas, "head_gain": head_gain, "w_out": w_out, "moe_tokens": moe_tokens, "moe_gain": moe_gain, "routes": routes, "route_weights": route_weights, "w_gate": w_gate, "w_up": w_up, "w_down": w_down}


eps = 1e-05
alpha_act = 1.702
limit_act = 7.0

def clamped_unit(gate, up):
    capped = jnp.minimum(gate, limit_act)
    linear = jnp.clip(up, -limit_act, limit_act)
    return capped * jax.nn.sigmoid(alpha_act * capped) * (linear + 1.0)

def hidden_rows(inputs, gate_matrix, up_matrix):
    gate = jnp.dot(inputs, gate_matrix, preferred_element_type=jnp.float32)
    up = jnp.dot(inputs, up_matrix, preferred_element_type=jnp.float32)
    return clamped_unit(gate, up).astype(jnp.bfloat16)

def map_weights(queries, keys, value_rows, query_pos, key_pos):
    scores = jnp.dot(queries, keys.T, preferred_element_type=jnp.float32) * HEAD ** (-0.5)
    visible = key_pos[None, :] <= query_pos[:, None]
    scores = jnp.where(visible, scores, -jnp.inf)
    peak = lax.optimization_barrier(jnp.max(scores, axis=1, keepdims=True))
    expo = jnp.where(visible, jnp.exp(scores - peak), 0.0)
    total = lax.optimization_barrier(jnp.sum(expo, axis=1, keepdims=True))
    mixed = jnp.dot(expo.astype(jnp.bfloat16), value_rows, preferred_element_type=jnp.float32)
    return mixed / total

def one_head(head, queries_a, queries_b, keys_a, keys_b, values, lambdas, head_gain):
    kv_head = head // (HEADS // KV_HEADS)
    query_a = lax.dynamic_slice_in_dim(queries_a, (head * HEAD).astype(jnp.int32), HEAD, 1)
    query_b = lax.dynamic_slice_in_dim(queries_b, (head * HEAD).astype(jnp.int32), HEAD, 1)
    key_a = lax.dynamic_slice_in_dim(keys_a, (kv_head * HEAD).astype(jnp.int32), HEAD, 1)
    key_b = lax.dynamic_slice_in_dim(keys_b, (kv_head * HEAD).astype(jnp.int32), HEAD, 1)
    value_head = lax.dynamic_slice_in_dim(values, (kv_head * VDIM).astype(jnp.int32), VDIM, 1)
    key_pos = jnp.arange(SEQ, dtype=jnp.int32)
    strength = lambdas[head]

    def one_block(index):
        start = (index * ATT_DEV).astype(jnp.int32)
        query_pos = start + jnp.arange(ATT_DEV, dtype=jnp.int32)
        first = map_weights(lax.dynamic_slice_in_dim(query_a, start, ATT_DEV, 0), key_a, value_head, query_pos, key_pos)
        second = map_weights(lax.dynamic_slice_in_dim(query_b, start, ATT_DEV, 0), key_b, value_head, query_pos, key_pos)
        diff = first - strength * second
        scaled = diff * lax.rsqrt(lax.optimization_barrier(jnp.mean(diff * diff, axis=-1, keepdims=True)) + eps) * head_gain
        return scaled.astype(jnp.bfloat16)
    return lax.map(one_block, jnp.arange(N_EP, dtype=jnp.int32)).reshape(SEQ, VDIM)

def reference(queries_a, queries_b, keys_a, keys_b, values, lambdas, head_gain, w_out, moe_tokens, moe_gain, routes, route_weights, w_gate, w_up, w_down):
    heads = lax.map(lambda head: one_head(head, queries_a, queries_b, keys_a, keys_b, values, lambdas, head_gain), jnp.arange(HEADS, dtype=jnp.int32))
    heads = heads.transpose(1, 0, 2).reshape(SEQ, N_TP, HEADS // N_TP * VDIM)
    weight_groups = w_out.reshape(N_TP, HEADS // N_TP * VDIM, D)
    head_parts = jnp.einsum('sjc,jcd->jsd', heads.astype(jnp.float32), weight_groups.astype(jnp.float32))
    head_parts = lax.optimization_barrier(head_parts.astype(jnp.bfloat16))
    mixer_out = lax.optimization_barrier(jnp.sum(head_parts.astype(jnp.float32), axis=0)).astype(jnp.bfloat16)
    inputs = moe_tokens.astype(jnp.float32)
    normed = (inputs * lax.rsqrt(lax.optimization_barrier(jnp.mean(inputs * inputs, axis=-1, keepdims=True)) + eps) * moe_gain).astype(jnp.bfloat16)
    blocks = MOE_TOK // TOKB
    chosen = routes.reshape(blocks, TOKB * TOP)
    member = (chosen[:, :, None] == jnp.arange(EXPERTS, dtype=jnp.int32)[None, None, :]).astype(jnp.int32)
    order_in = lax.optimization_barrier(jnp.sum(jnp.cumsum(member, axis=1) * member, axis=2)) - 1
    block_ids = jnp.arange(blocks, dtype=jnp.int32)[:, None]
    slot_ids = ((chosen * blocks + block_ids) * CAP + order_in).astype(jnp.int32)
    token_ids = (block_ids * TOKB + jnp.arange(TOKB * TOP, dtype=jnp.int32)[None, :] // TOP).astype(jnp.int32)
    owner = jnp.full((EXPERTS * blocks * CAP,), MOE_TOK, jnp.int32).at[slot_ids.reshape(-1)].set(token_ids.reshape(-1))
    owner = owner.reshape(EXPERTS, blocks * CAP)

    def one_expert(index):
        slot_owner = owner[index]
        valid = slot_owner < MOE_TOK
        taken = jnp.take(normed, jnp.minimum(slot_owner, MOE_TOK - 1), axis=0)
        taken = jnp.where(valid[:, None], taken, jnp.zeros_like(taken))
        hidden = hidden_rows(taken, w_gate[index], w_up[index])
        unit_parts = jnp.einsum('rjf,jfd->jrd', hidden.reshape(-1, N_TP, FF // N_TP).astype(jnp.float32), w_down[index].reshape(N_TP, FF // N_TP, D).astype(jnp.float32))
        unit_parts = lax.optimization_barrier(unit_parts.astype(jnp.bfloat16))
        return lax.optimization_barrier(jnp.sum(unit_parts.astype(jnp.float32), axis=0)).astype(jnp.bfloat16)
    expert_rows = lax.map(one_expert, jnp.arange(EXPERTS, dtype=jnp.int32))
    picked = jnp.take(expert_rows.reshape(-1, D), slot_ids.reshape(-1), axis=0).reshape(MOE_TOK, TOP, D)
    moe_out = lax.optimization_barrier(jnp.sum(picked.astype(jnp.float32) * route_weights[:, :, None], axis=1)).astype(jnp.bfloat16)
    return (mixer_out, moe_out)
```

```python
import functools

import jax
import jax.numpy as jnp
from jax import lax
from jax.experimental import pallas as pl
from jax.experimental.pallas import tpu as pltpu
from jax.sharding import PartitionSpec as P

HEAD = 64
VDIM = 128
TOP = 2


eps = 1e-05
alpha_act = 1.702
limit_act = 7.0
negative = -1e30


def clamped_unit(gate, up):
    capped = jnp.minimum(gate, limit_act)
    linear = jnp.clip(up, -limit_act, limit_act)
    return capped * jax.nn.sigmoid(alpha_act * capped) * (linear + 1.0)


def hidden_rows(inputs, gate_matrix, up_matrix):
    gate = jnp.dot(inputs, gate_matrix, preferred_element_type=jnp.float32)
    up = jnp.dot(inputs, up_matrix, preferred_element_type=jnp.float32)
    return clamped_unit(gate, up).astype(jnp.bfloat16)


def pick_rows(table, owner):
    valid = owner < table.shape[0]
    chosen = jnp.take(table, jnp.minimum(owner, table.shape[0] - 1), axis=0)
    return jnp.where(valid[:, None], chosen, jnp.zeros_like(chosen))


def mixer(queries_a, queries_b, keys_a, keys_b, values, lambdas, head_gain, w_out):
    tokens = queries_a.shape[0]
    local_heads = lambdas.shape[0]
    kv_local = keys_a.shape[1] // HEAD
    group = local_heads // kv_local
    scale = HEAD ** (-0.5)
    query_pos = lax.axis_index("ep") * tokens + jnp.arange(tokens, dtype=jnp.int32)
    grouped_a = queries_a.reshape(tokens, kv_local, group, HEAD)
    grouped_b = queries_b.reshape(tokens, kv_local, group, HEAD)
    lowest = jnp.full((kv_local, group, tokens), negative, jnp.float32)
    nothing = jnp.zeros((kv_local, group, tokens), jnp.float32)
    blank = jnp.zeros((kv_local, group, tokens, VDIM), jnp.float32)

    def one_map(grouped, keys, value_rows, visible, state):
        peak, total, accum = state
        scores = (
            jnp.einsum("rgjd,ngd->gjrn", grouped, keys, preferred_element_type=jnp.float32) * scale
        )
        scores = jnp.where(visible, scores, negative)
        new_peak = jnp.maximum(peak, jnp.max(scores, axis=-1))
        expo = jnp.where(visible, jnp.exp(scores - new_peak[..., None]), 0.0)
        total = jnp.sum(expo, axis=-1)
        accum = jnp.einsum(
            "gjrn,ngv->gjrv",
            expo.astype(jnp.bfloat16),
            value_rows,
            preferred_element_type=jnp.float32,
        )
        return (new_peak, total, accum)

    initial = (lowest, nothing, blank, lowest, nothing, blank)
    piece_a = lax.all_gather(keys_a, "ep", axis=0, tiled=True)
    piece_b = lax.all_gather(keys_b, "ep", axis=0, tiled=True)
    piece_v = lax.all_gather(values, "ep", axis=0, tiled=True)
    count = piece_a.shape[0]

    def visit(state):
        key_pos = jnp.arange(count, dtype=jnp.int32)
        visible = key_pos[None, :] <= query_pos[:, None]
        value_rows = piece_v.reshape(count, kv_local, VDIM)
        first = one_map(
            grouped_a, piece_a.reshape(count, kv_local, HEAD), value_rows, visible, state[:3]
        )
        second = one_map(
            grouped_b, piece_b.reshape(count, kv_local, HEAD), value_rows, visible, state[3:]
        )
        return first + second

    result = lax.cond(jnp.int32(0) <= query_pos[tokens - 1], visit, lambda state: state, initial)
    mixed_a = result[2] / result[1][..., None]
    mixed_b = result[5] / result[4][..., None]
    diff = mixed_a - lambdas.reshape(kv_local, group, 1, 1) * mixed_b
    heads_out = (
        diff * lax.rsqrt(jnp.mean(diff * diff, axis=-1, keepdims=True) + eps) * head_gain
    ).astype(jnp.bfloat16)
    weights_out = w_out.reshape(kv_local, group, VDIM, w_out.shape[1])
    return lax.psum_scatter(
        jnp.einsum(
            "gjrv,gjvd->rd", heads_out, weights_out, preferred_element_type=jnp.float32
        ).astype(jnp.bfloat16),
        "tp",
        scatter_dimension=0,
        tiled=True,
    )


def experts(moe_tokens, moe_gain, routes, route_weights, w_gate, w_up, w_down):
    tok_rows, width = moe_tokens.shape
    n_experts = lax.axis_size("ep") * w_gate.shape[0]
    capacity = max(2, 3 * tok_rows * TOP // (2 * n_experts))
    inputs = moe_tokens.astype(jnp.float32)
    normed = (
        inputs * lax.rsqrt(jnp.mean(inputs * inputs, axis=-1, keepdims=True) + eps) * moe_gain
    ).astype(jnp.bfloat16)
    chosen = routes.reshape(-1)
    member = (chosen[:, None] == jnp.arange(n_experts, dtype=jnp.int32)[None, :]).astype(jnp.int32)
    order_in = jnp.sum(jnp.cumsum(member, axis=0) * member, axis=1) - 1
    slot_ids = chosen * capacity + order_in
    owner = (
        jnp.full((n_experts * capacity,), tok_rows, jnp.int32)
        .at[slot_ids]
        .set(jnp.arange(tok_rows * TOP, dtype=jnp.int32) // TOP)
    )
    outgoing = pick_rows(normed, owner).reshape(n_experts, capacity, width)
    arrived = lax.all_to_all(outgoing, "ep", split_axis=0, concat_axis=1, tiled=True).reshape(
        -1, width
    )
    hidden = hidden_rows(lax.all_gather(arrived, "tp", axis=0, tiled=True), w_gate[0], w_up[0])
    expert_out = lax.psum_scatter(
        jnp.dot(hidden, w_down[0], preferred_element_type=jnp.float32).astype(jnp.bfloat16),
        "tp",
        scatter_dimension=0,
        tiled=True,
    )
    returned = lax.all_to_all(
        expert_out.reshape(-1, capacity, width), "ep", split_axis=0, concat_axis=0, tiled=True
    )
    picked = jnp.take(returned.reshape(-1, width), slot_ids, axis=0).reshape(tok_rows, TOP, width)
    return jnp.sum(picked.astype(jnp.float32) * route_weights[:, :, None], axis=1).astype(
        jnp.bfloat16
    )


def body(
    queries_a,
    queries_b,
    keys_a,
    keys_b,
    values,
    lambdas,
    head_gain,
    w_out,
    moe_tokens,
    moe_gain,
    routes,
    route_weights,
    w_gate,
    w_up,
    w_down,
):
    mixer_out = mixer(queries_a, queries_b, keys_a, keys_b, values, lambdas, head_gain, w_out)
    moe_out = experts(moe_tokens, moe_gain, routes, route_weights, w_gate, w_up, w_down)
    return (mixer_out, moe_out)


MESH = pl.DeviceIdType.MESH
OUT, CORE, ACROSS, CORE_ACROSS, PART, PAIR, SUMS, BACK, KV_Z, KV_Y = range(10)


def xor(first, second, limit):
    total, bit = 0, 1
    while bit < limit:
        total = total + (first // bit + second // bit) % 2 * bit
        bit *= 2
    return total


def exchange(
    n, outgoing, kv, w_gate, w_up, w_down, ret, kv_all,
    rows, parts, part_in, pair_in, sums_in, sums, final, hidden, gate_v, up_v, down_v,
    send, recv, local,
):
    me = lax.axis_index("ep")
    tp = lax.axis_index("tp")
    core = tp + 1 - 2 * (tp % 2)
    across = tp + 2 - 4 * (tp // 2)
    cap, width = outgoing.shape[1:]
    units = hidden.shape[1]
    flat = 4 * cap

    def mask_of(k):
        return 2 * ((n // 2 - k // 2) % (n // 2)) + k % 2

    def partner(k):
        return xor(me, mask_of(k), n)

    def copy(kind, k, source, target, device):
        return pltpu.make_async_remote_copy(
            src_ref=source,
            dst_ref=target,
            send_sem=send.at[kind, k],
            recv_sem=recv.at[kind, k],
            device_id=device,
            device_id_type=MESH,
        )

    def out_copy(k):
        return copy(OUT, k, outgoing.at[partner(k)], rows.at[k, 0], {"ep": partner(k)})

    def core_copy(k):
        return copy(CORE, k, rows.at[k, 0], rows.at[k, 1], {"tp": core})

    def across_copy(k):
        return copy(ACROSS, k, rows.at[k, 0], rows.at[k, 2], {"tp": across})

    def core_across_copy(k):
        return copy(CORE_ACROSS, k, rows.at[k, 2], rows.at[k, 3], {"tp": core})

    def part_copy(k):
        return copy(PART, k, parts.at[k, 1], part_in.at[k], {"tp": core})

    def pair_copy(k):
        return copy(PAIR, k, parts.at[k, 3], pair_in.at[k], {"tp": core})

    def sums_copy(k):
        return copy(SUMS, k, sums.at[k], sums_in.at[k], {"tp": across})

    def back_copy(k):
        return copy(BACK, k, final.at[k], ret.at[me], {"ep": partner(k)})

    def kv_z_copy(z):
        return copy(KV_Z, z, kv, kv_all.at[me], {"ep": xor(me, 2 * z, n)})

    def kv_y_copy(z):
        source = xor(me, 2 * z, n)
        return copy(KV_Y, z, kv_all.at[source], kv_all.at[source], {"ep": xor(me, 1, n)})

    own = pltpu.make_async_copy(outgoing.at[me], rows.at[0, 0], local.at[0])
    own.start()
    own_kv = pltpu.make_async_copy(kv, kv_all.at[me], local.at[1])
    own_kv.start()
    loads = [
        pltpu.make_async_copy(w_gate, gate_v, local.at[2]),
        pltpu.make_async_copy(w_up, up_v, local.at[3]),
        pltpu.make_async_copy(w_down, down_v, local.at[4]),
    ]
    for load in loads:
        load.start()

    barrier = pltpu.get_barrier_semaphore()
    for shift in range(1, n):
        pl.semaphore_signal(
            barrier, inc=1, device_id={"ep": (me + shift) % n}, device_id_type=MESH
        )
    for shift in range(1, 4):
        pl.semaphore_signal(
            barrier, inc=1, device_id={"tp": (tp + shift) % 4}, device_id_type=MESH
        )
    pl.semaphore_wait(barrier, n + 2)

    own.wait()
    core_copy(0).start()
    across_copy(0).start()

    @pl.loop(1, n)
    def _(k):
        out_copy(k).start()

    for z in range(1, n // 2):
        kv_z_copy(z).start()
    own_kv.wait()
    for load in loads:
        load.wait()

    @pl.loop(0, n + 2)
    def _(k):
        @pl.when(k + 1 < n)
        def _():
            out_copy(k + 1).wait_recv()
            core_copy(k + 1).start()
            across_copy(k + 1).start()

        @pl.when(k < n)
        def _():
            across_copy(k).wait_recv()
            core_across_copy(k).start()
            core_copy(k).wait_recv()
            core_across_copy(k).wait_recv()
            inputs = rows[k].reshape(flat, width)
            step = min(256, units)
            for first in range(0, units, step):
                gate = jnp.dot(
                    inputs, gate_v[:, first : first + step], preferred_element_type=jnp.float32
                )
                up = jnp.dot(
                    inputs, up_v[:, first : first + step], preferred_element_type=jnp.float32
                )
                hidden[:, first : first + step] = clamped_unit(gate, up).astype(jnp.bfloat16)
            for first in range(0, width, 256):
                piece = jnp.dot(
                    hidden[...], down_v[:, first : first + 256], preferred_element_type=jnp.float32
                )
                parts[k, :, :, first : first + 256] = piece.astype(jnp.bfloat16).reshape(
                    4, cap, 256
                )
            pair_copy(k).start()
            part_copy(k).start()

        @pl.when((k >= 1) & (k <= n))
        def _():
            j = k - 1
            pair_copy(j).wait_recv()
            sums[j] = (
                parts[j, 2].astype(jnp.float32) + pair_in[j].astype(jnp.float32)
            ).astype(jnp.bfloat16)
            sums_copy(j).start()

        @pl.when(k >= 2)
        def _():
            j = k - 2
            part_copy(j).wait_recv()
            sums_copy(j).wait_recv()
            final[j] = (
                parts[j, 0].astype(jnp.float32)
                + part_in[j].astype(jnp.float32)
                + sums_in[j].astype(jnp.float32)
            ).astype(jnp.bfloat16)

            @pl.when(j >= 1)
            def _():
                back_copy(j).start()

        @pl.when(k == n // 2)
        def _():
            for z in range(n // 2):
                if z:
                    kv_z_copy(z).wait_recv()
                kv_y_copy(z).start()

    ret[me] = final[0]
    for z in range(n // 2):
        if z:
            kv_z_copy(z).wait_send()
        kv_y_copy(z).wait_send()
        kv_y_copy(z).wait_recv()

    @pl.loop(0, n)
    def _(k):
        for made in (core_copy, across_copy, core_across_copy, part_copy, pair_copy, sums_copy):
            made(k).wait_send()

        @pl.when(k >= 1)
        def _():
            out_copy(k).wait_send()
            back_copy(k).wait_send()
            back_copy(k).wait_recv()


def run_exchange(n, outgoing, kv, w_gate, w_up, w_down):
    _, cap, width = outgoing.shape
    units = w_gate.shape[1]
    block = (n, cap, width)
    vmem = pl.BlockSpec(memory_space=pltpu.VMEM)
    hbm = pl.BlockSpec(memory_space=pl.ANY)
    return pl.pallas_call(
        functools.partial(exchange, n),
        out_shape=(
            jax.ShapeDtypeStruct(block, jnp.bfloat16),
            jax.ShapeDtypeStruct((n,) + kv.shape, jnp.bfloat16),
        ),
        in_specs=[vmem, vmem, hbm, hbm, hbm],
        out_specs=(vmem, vmem),
        scratch_shapes=[
            pltpu.VMEM((n, 4, cap, width), jnp.bfloat16),
            pltpu.VMEM((n, 4, cap, width), jnp.bfloat16),
            pltpu.VMEM(block, jnp.bfloat16),
            pltpu.VMEM(block, jnp.bfloat16),
            pltpu.VMEM(block, jnp.bfloat16),
            pltpu.VMEM(block, jnp.bfloat16),
            pltpu.VMEM(block, jnp.bfloat16),
            pltpu.VMEM((4 * cap, units), jnp.bfloat16),
            pltpu.VMEM(w_gate.shape, jnp.bfloat16),
            pltpu.VMEM(w_up.shape, jnp.bfloat16),
            pltpu.VMEM(w_down.shape, jnp.bfloat16),
            pltpu.SemaphoreType.DMA((10, n)),
            pltpu.SemaphoreType.DMA((10, n)),
            pltpu.SemaphoreType.DMA((5,)),
        ],
        compiler_params=pltpu.CompilerParams(
            collective_id=0, has_side_effects=True, vmem_limit_bytes=60 * 2**20
        ),
        name="exchange",
    )(outgoing, kv, w_gate, w_up, w_down)


def scatter_sum(n, parts, out, landed, send, recv):
    me = lax.axis_index("tp")
    barrier = pltpu.get_barrier_semaphore()
    for shift in range(1, n):
        pl.semaphore_signal(
            barrier, inc=1, device_id={"tp": (me + shift) % n}, device_id_type=MESH
        )
    pl.semaphore_wait(barrier, n - 1)
    copies = []
    for shift in range(1, n):
        target = (me + shift) % n
        copies.append(
            pltpu.make_async_remote_copy(
                src_ref=parts.at[target],
                dst_ref=landed.at[shift - 1],
                send_sem=send.at[shift - 1],
                recv_sem=recv.at[shift - 1],
                device_id={"tp": target},
                device_id_type=MESH,
            )
        )
        copies[-1].start()
    total = parts[me].astype(jnp.float32)
    for shift in range(1, n):
        copies[shift - 1].wait_recv()
        total = total + landed[shift - 1].astype(jnp.float32)
    out[...] = total.astype(jnp.bfloat16)
    for made in copies:
        made.wait_send()


def run_scatter_sum(n, parts):
    count, width = parts.shape[0] // n, parts.shape[1]
    vmem = pl.BlockSpec(memory_space=pltpu.VMEM)
    return pl.pallas_call(
        functools.partial(scatter_sum, n),
        out_shape=jax.ShapeDtypeStruct((count, width), jnp.bfloat16),
        in_specs=[vmem],
        out_specs=vmem,
        scratch_shapes=[
            pltpu.VMEM((n - 1, count, width), jnp.bfloat16),
            pltpu.SemaphoreType.DMA((n - 1,)),
            pltpu.SemaphoreType.DMA((n - 1,)),
        ],
        compiler_params=pltpu.CompilerParams(collective_id=1, has_side_effects=True),
        name="scatter_sum",
    )(parts.reshape(n, count, width))


def attend(queries_a, queries_b, kv_all, lambdas, head_gain, w_out, n_tp):
    tokens = queries_a.shape[0]
    local_heads = lambdas.shape[0]
    kv_rows = kv_all.reshape(-1, kv_all.shape[-1])
    count = kv_rows.shape[0]
    kv_local = kv_rows.shape[1] // (2 * HEAD + VDIM)
    group = local_heads // kv_local
    scale = HEAD ** (-0.5)
    span = kv_local * HEAD
    query_pos = lax.axis_index("ep") * tokens + jnp.arange(tokens, dtype=jnp.int32)
    key_pos = jnp.arange(count, dtype=jnp.int32)
    visible = key_pos[None, :] <= query_pos[:, None]
    value_rows = kv_rows[:, 2 * span :].reshape(count, kv_local, VDIM)

    def one_map(queries, keys):
        grouped = queries.reshape(tokens, kv_local, group, HEAD)
        scores = (
            jnp.einsum(
                "rgjd,ngd->gjrn",
                grouped,
                keys.reshape(count, kv_local, HEAD),
                preferred_element_type=jnp.float32,
            )
            * scale
        )
        scores = jnp.where(visible, scores, negative)
        peak = jnp.max(scores, axis=-1, keepdims=True)
        expo = jnp.where(visible, jnp.exp(scores - peak), 0.0)
        total = jnp.sum(expo, axis=-1, keepdims=True)
        mixed = jnp.einsum(
            "gjrn,ngv->gjrv",
            expo.astype(jnp.bfloat16),
            value_rows,
            preferred_element_type=jnp.float32,
        )
        return mixed / total

    first = one_map(queries_a, kv_rows[:, :span])
    second = one_map(queries_b, kv_rows[:, span : 2 * span])
    diff = first - lambdas.reshape(kv_local, group, 1, 1) * second
    heads_out = (
        diff * lax.rsqrt(jnp.mean(diff * diff, axis=-1, keepdims=True) + eps) * head_gain
    ).astype(jnp.bfloat16)
    weights_out = w_out.reshape(kv_local, group, VDIM, w_out.shape[1])
    parts = jnp.einsum(
        "gjrv,gjvd->rd", heads_out, weights_out, preferred_element_type=jnp.float32
    ).astype(jnp.bfloat16)
    return run_scatter_sum(n_tp, parts)


def fast_body(
    queries_a, queries_b, keys_a, keys_b, values, lambdas, head_gain, w_out,
    moe_tokens, moe_gain, routes, route_weights, w_gate, w_up, w_down,
):
    n, n_tp = lax.axis_size("ep"), lax.axis_size("tp")
    tok_rows, width = moe_tokens.shape
    cap = 3 * tok_rows * TOP // (2 * n)
    inputs = moe_tokens.astype(jnp.float32)
    normed = (
        inputs * lax.rsqrt(jnp.mean(inputs * inputs, axis=-1, keepdims=True) + eps) * moe_gain
    ).astype(jnp.bfloat16)
    named = routes[:, :, None] == jnp.arange(n, dtype=jnp.int32)[None, None, :]
    member = jnp.any(named, axis=1)
    earlier = jnp.tril(jnp.ones((tok_rows, tok_rows), jnp.bfloat16), -1)
    place = jnp.dot(
        earlier, member.astype(jnp.bfloat16), preferred_element_type=jnp.float32
    ).astype(jnp.int32)
    slot = jnp.where(member, place, cap).T
    pick = (slot[:, None, :] == jnp.arange(cap, dtype=jnp.int32)[None, :, None]).reshape(
        n * cap, tok_rows
    )
    outgoing = (
        jnp.dot(pick.astype(jnp.bfloat16), normed, preferred_element_type=jnp.float32)
        .astype(jnp.bfloat16)
        .reshape(n, cap, width)
    )
    kv = jnp.concatenate([keys_a, keys_b, values], axis=1)
    returned, kv_all = run_exchange(n, outgoing, kv, w_gate[0], w_up[0], w_down[0])
    mixer_out = attend(queries_a, queries_b, kv_all, lambdas, head_gain, w_out, n_tp)
    slot_ids = routes * cap + jnp.sum(jnp.where(named, place[:, None, :], 0), axis=2)
    table = returned.reshape(n * cap, width)
    total = 0.0
    for k in range(TOP):
        chosen = slot_ids[:, k : k + 1] == jnp.arange(n * cap, dtype=jnp.int32)[None, :]
        total = total + route_weights[:, k : k + 1] * jnp.dot(
            chosen.astype(jnp.bfloat16), table, preferred_element_type=jnp.float32
        )
    return (mixer_out, total.astype(jnp.bfloat16))


def whole_body(*args):
    n, n_tp = lax.axis_size("ep"), lax.axis_size("tp")
    tok_rows, w_gate = args[8].shape[0], args[12]
    cap = 3 * tok_rows * TOP // (2 * n)
    if w_gate.shape[0] == 1 and n_tp == 4 and n & (n - 1) == 0 and n >= 4 and cap % 16 == 0:
        return fast_body(*args)
    return body(*args)


def solution(mesh):
    return jax.shard_map(
        whole_body,
        mesh=mesh,
        in_specs=(
            P("ep", "tp"),
            P("ep", "tp"),
            P("ep", "tp"),
            P("ep", "tp"),
            P("ep", "tp"),
            P("tp"),
            P(),
            P("tp", None),
            P(("ep", "tp"), None),
            P(),
            P(("ep", "tp"), None),
            P(("ep", "tp"), None),
            P("ep", None, "tp"),
            P("ep", None, "tp"),
            P("ep", "tp", None),
        ),
        out_specs=(P(("ep", "tp"), None), P(("ep", "tp"), None)),
        check_vma=False,
    )
```

```python
import functools

import jax
import jax.numpy as jnp
from jax import lax
from jax.experimental import pallas as pl
from jax.experimental.pallas import tpu as pltpu
from jax.sharding import PartitionSpec as P

HEAD = 64
VDIM = 128
TOP = 2


eps = 1e-05
alpha_act = 1.702
limit_act = 7.0
negative = -1e30


def clamped_unit(gate, up):
    capped = jnp.minimum(gate, limit_act)
    linear = jnp.clip(up, -limit_act, limit_act)
    return capped * jax.nn.sigmoid(alpha_act * capped) * (linear + 1.0)


def hidden_rows(inputs, gate_matrix, up_matrix):
    gate = jnp.dot(inputs, gate_matrix, preferred_element_type=jnp.float32)
    up = jnp.dot(inputs, up_matrix, preferred_element_type=jnp.float32)
    return clamped_unit(gate, up).astype(jnp.bfloat16)


def pick_rows(table, owner):
    valid = owner < table.shape[0]
    chosen = jnp.take(table, jnp.minimum(owner, table.shape[0] - 1), axis=0)
    return jnp.where(valid[:, None], chosen, jnp.zeros_like(chosen))


def mixer(queries_a, queries_b, keys_a, keys_b, values, lambdas, head_gain, w_out):
    tokens = queries_a.shape[0]
    local_heads = lambdas.shape[0]
    kv_local = keys_a.shape[1] // HEAD
    group = local_heads // kv_local
    scale = HEAD ** (-0.5)
    query_pos = lax.axis_index("ep") * tokens + jnp.arange(tokens, dtype=jnp.int32)
    grouped_a = queries_a.reshape(tokens, kv_local, group, HEAD)
    grouped_b = queries_b.reshape(tokens, kv_local, group, HEAD)
    lowest = jnp.full((kv_local, group, tokens), negative, jnp.float32)
    nothing = jnp.zeros((kv_local, group, tokens), jnp.float32)
    blank = jnp.zeros((kv_local, group, tokens, VDIM), jnp.float32)

    def one_map(grouped, keys, value_rows, visible, state):
        peak, total, accum = state
        scores = (
            jnp.einsum("rgjd,ngd->gjrn", grouped, keys, preferred_element_type=jnp.float32) * scale
        )
        scores = jnp.where(visible, scores, negative)
        new_peak = jnp.maximum(peak, jnp.max(scores, axis=-1))
        expo = jnp.where(visible, jnp.exp(scores - new_peak[..., None]), 0.0)
        total = jnp.sum(expo, axis=-1)
        accum = jnp.einsum(
            "gjrn,ngv->gjrv",
            expo.astype(jnp.bfloat16),
            value_rows,
            preferred_element_type=jnp.float32,
        )
        return (new_peak, total, accum)

    initial = (lowest, nothing, blank, lowest, nothing, blank)
    piece_a = lax.all_gather(keys_a, "ep", axis=0, tiled=True)
    piece_b = lax.all_gather(keys_b, "ep", axis=0, tiled=True)
    piece_v = lax.all_gather(values, "ep", axis=0, tiled=True)
    count = piece_a.shape[0]

    def visit(state):
        key_pos = jnp.arange(count, dtype=jnp.int32)
        visible = key_pos[None, :] <= query_pos[:, None]
        value_rows = piece_v.reshape(count, kv_local, VDIM)
        first = one_map(
            grouped_a, piece_a.reshape(count, kv_local, HEAD), value_rows, visible, state[:3]
        )
        second = one_map(
            grouped_b, piece_b.reshape(count, kv_local, HEAD), value_rows, visible, state[3:]
        )
        return first + second

    result = lax.cond(jnp.int32(0) <= query_pos[tokens - 1], visit, lambda state: state, initial)
    mixed_a = result[2] / result[1][..., None]
    mixed_b = result[5] / result[4][..., None]
    diff = mixed_a - lambdas.reshape(kv_local, group, 1, 1) * mixed_b
    heads_out = (
        diff * lax.rsqrt(jnp.mean(diff * diff, axis=-1, keepdims=True) + eps) * head_gain
    ).astype(jnp.bfloat16)
    weights_out = w_out.reshape(kv_local, group, VDIM, w_out.shape[1])
    return lax.psum_scatter(
        jnp.einsum(
            "gjrv,gjvd->rd", heads_out, weights_out, preferred_element_type=jnp.float32
        ).astype(jnp.bfloat16),
        "tp",
        scatter_dimension=0,
        tiled=True,
    )


def experts(moe_tokens, moe_gain, routes, route_weights, w_gate, w_up, w_down):
    tok_rows, width = moe_tokens.shape
    n_experts = lax.axis_size("ep") * w_gate.shape[0]
    capacity = max(2, 3 * tok_rows * TOP // (2 * n_experts))
    inputs = moe_tokens.astype(jnp.float32)
    normed = (
        inputs * lax.rsqrt(jnp.mean(inputs * inputs, axis=-1, keepdims=True) + eps) * moe_gain
    ).astype(jnp.bfloat16)
    chosen = routes.reshape(-1)
    member = (chosen[:, None] == jnp.arange(n_experts, dtype=jnp.int32)[None, :]).astype(jnp.int32)
    order_in = jnp.sum(jnp.cumsum(member, axis=0) * member, axis=1) - 1
    slot_ids = chosen * capacity + order_in
    owner = (
        jnp.full((n_experts * capacity,), tok_rows, jnp.int32)
        .at[slot_ids]
        .set(jnp.arange(tok_rows * TOP, dtype=jnp.int32) // TOP)
    )
    outgoing = pick_rows(normed, owner).reshape(n_experts, capacity, width)
    arrived = lax.all_to_all(outgoing, "ep", split_axis=0, concat_axis=1, tiled=True).reshape(
        -1, width
    )
    hidden = hidden_rows(lax.all_gather(arrived, "tp", axis=0, tiled=True), w_gate[0], w_up[0])
    expert_out = lax.psum_scatter(
        jnp.dot(hidden, w_down[0], preferred_element_type=jnp.float32).astype(jnp.bfloat16),
        "tp",
        scatter_dimension=0,
        tiled=True,
    )
    returned = lax.all_to_all(
        expert_out.reshape(-1, capacity, width), "ep", split_axis=0, concat_axis=0, tiled=True
    )
    picked = jnp.take(returned.reshape(-1, width), slot_ids, axis=0).reshape(tok_rows, TOP, width)
    return jnp.sum(picked.astype(jnp.float32) * route_weights[:, :, None], axis=1).astype(
        jnp.bfloat16
    )


def body(
    queries_a,
    queries_b,
    keys_a,
    keys_b,
    values,
    lambdas,
    head_gain,
    w_out,
    moe_tokens,
    moe_gain,
    routes,
    route_weights,
    w_gate,
    w_up,
    w_down,
):
    mixer_out = mixer(queries_a, queries_b, keys_a, keys_b, values, lambdas, head_gain, w_out)
    moe_out = experts(moe_tokens, moe_gain, routes, route_weights, w_gate, w_up, w_down)
    return (mixer_out, moe_out)


MESH = pl.DeviceIdType.MESH
OUT, CORE, ACROSS, CORE_ACROSS, PART, PAIR, SUMS, BACK, KV_Z, KV_Y, MIX = range(11)


def xor(first, second, limit):
    total, bit = 0, 1
    while bit < limit:
        total = total + (first // bit + second // bit) % 2 * bit
        bit *= 2
    return total


def exchange(
    n, outgoing, kv, queries_a, queries_b, head_gain, lambdas, w_gate, w_up, w_down, w_out,
    ret, mixer_out,
    rows, parts, part_in, pair_in, sums_in, sums, final, hidden, gate_v, up_v, down_v, out_v,
    kv_all, heads, shares, landed, send, recv, local,
):
    me = lax.axis_index("ep")
    tp = lax.axis_index("tp")
    core = tp + 1 - 2 * (tp % 2)
    across = tp + 2 - 4 * (tp // 2)
    cap, width = outgoing.shape[1:]
    units = hidden.shape[1]
    flat = 4 * cap

    def mask_of(k):
        return 2 * ((n // 2 - k // 2) % (n // 2)) + k % 2

    def partner(k):
        return xor(me, mask_of(k), n)

    def copy(kind, k, source, target, device):
        return pltpu.make_async_remote_copy(
            src_ref=source,
            dst_ref=target,
            send_sem=send.at[kind, k],
            recv_sem=recv.at[kind, k],
            device_id=device,
            device_id_type=MESH,
        )

    def out_copy(k):
        return copy(OUT, k, outgoing.at[partner(k)], rows.at[k, 0], {"ep": partner(k)})

    def core_copy(k):
        return copy(CORE, k, rows.at[k, 0], rows.at[k, 1], {"tp": core})

    def across_copy(k):
        return copy(ACROSS, k, rows.at[k, 0], rows.at[k, 2], {"tp": across})

    def core_across_copy(k):
        return copy(CORE_ACROSS, k, rows.at[k, 2], rows.at[k, 3], {"tp": core})

    def part_copy(k):
        return copy(PART, k, parts.at[k, 1], part_in.at[k], {"tp": core})

    def pair_copy(k):
        return copy(PAIR, k, parts.at[k, 3], pair_in.at[k], {"tp": core})

    def sums_copy(k):
        return copy(SUMS, k, sums.at[k], sums_in.at[k], {"tp": across})

    def back_copy(k):
        return copy(BACK, k, final.at[k], ret.at[me], {"ep": partner(k)})

    def kv_z_copy(z):
        return copy(KV_Z, z, kv, kv_all.at[me], {"ep": xor(me, 2 * z, n)})

    def kv_y_copy(z):
        source = xor(me, 2 * z, n)
        return copy(KV_Y, z, kv_all.at[source], kv_all.at[source], {"ep": xor(me, 1, n)})

    def mix_copy(shift):
        target = (tp + shift) % 4
        return copy(MIX, shift, shares.at[target], landed.at[shift - 1], {"tp": target})

    tokens = kv.shape[0]
    local_heads = heads.shape[1] // VDIM
    kv_local = kv.shape[1] // (2 * HEAD + VDIM)
    span = kv_local * HEAD

    def one_map(queries, head, offset):
        g = head // (local_heads // kv_local)
        count = n * tokens
        first = offset + g * HEAD
        keys = kv_all[:, :, first : first + HEAD].reshape(count, HEAD)
        first = 2 * span + g * VDIM
        value_rows = kv_all[:, :, first : first + VDIM].reshape(count, VDIM)
        scores = lax.dot_general(
            queries[:, head * HEAD : (head + 1) * HEAD],
            keys,
            (((1,), (1,)), ((), ())),
            preferred_element_type=jnp.float32,
        ) * HEAD ** (-0.5)
        query_pos = me * tokens + lax.broadcasted_iota(jnp.int32, scores.shape, 0)
        key_pos = lax.broadcasted_iota(jnp.int32, scores.shape, 1)
        scores = jnp.where(key_pos <= query_pos, scores, negative)
        expo = jnp.exp(scores - jnp.max(scores, axis=1, keepdims=True))
        total = jnp.sum(expo, axis=1, keepdims=True)
        mixed = jnp.dot(
            expo.astype(jnp.bfloat16), value_rows, preferred_element_type=jnp.float32
        )
        return mixed / total

    def attend(head):
        diff = one_map(queries_a, head, 0) - lambdas[head] * one_map(queries_b, head, span)
        norm = lax.rsqrt(jnp.mean(diff * diff, axis=1, keepdims=True) + eps)
        heads[:, head * VDIM : (head + 1) * VDIM] = (diff * norm * head_gain[...]).astype(
            jnp.bfloat16
        )

    own = pltpu.make_async_copy(outgoing.at[me], rows.at[0, 0], local.at[0])
    own.start()
    own_kv = pltpu.make_async_copy(kv, kv_all.at[me], local.at[1])
    own_kv.start()
    loads = [
        pltpu.make_async_copy(w_gate, gate_v, local.at[2]),
        pltpu.make_async_copy(w_up, up_v, local.at[3]),
        pltpu.make_async_copy(w_down, down_v, local.at[4]),
        pltpu.make_async_copy(w_out, out_v, local.at[5]),
    ]
    for load in loads:
        load.start()

    barrier = pltpu.get_barrier_semaphore()
    for shift in range(1, n):
        pl.semaphore_signal(
            barrier, inc=1, device_id={"ep": (me + shift) % n}, device_id_type=MESH
        )
    for shift in range(1, 4):
        pl.semaphore_signal(
            barrier, inc=1, device_id={"tp": (tp + shift) % 4}, device_id_type=MESH
        )
    pl.semaphore_wait(barrier, n + 2)

    own.wait()
    core_copy(0).start()
    across_copy(0).start()

    for k in range(1, 4):
        out_copy(k).start()
    for z in range(1, n // 2):
        kv_z_copy(z).start()

    @pl.loop(4, n)
    def _(k):
        out_copy(k).start()

    own_kv.wait()
    for load in loads:
        load.wait()

    @pl.loop(0, n + 2)
    def _(k):
        @pl.when(k + 1 < n)
        def _():
            out_copy(k + 1).wait_recv()
            core_copy(k + 1).start()
            across_copy(k + 1).start()

        @pl.when(k < n)
        def _():
            across_copy(k).wait_recv()
            core_across_copy(k).start()

        @pl.when((k >= 1) & (k <= n))
        def _():
            j = k - 1
            pair_copy(j).wait_recv()
            sums[j] = (
                parts[j, 2].astype(jnp.float32) + pair_in[j].astype(jnp.float32)
            ).astype(jnp.bfloat16)
            sums_copy(j).start()

        @pl.when(k >= 2)
        def _():
            j = k - 2
            part_copy(j).wait_recv()
            sums_copy(j).wait_recv()
            final[j] = (
                parts[j, 0].astype(jnp.float32)
                + part_in[j].astype(jnp.float32)
                + sums_in[j].astype(jnp.float32)
            ).astype(jnp.bfloat16)

            @pl.when(j >= 1)
            def _():
                back_copy(j).start()

        @pl.when(k < n)
        def _():
            core_copy(k).wait_recv()
            core_across_copy(k).wait_recv()
            inputs = rows[k].reshape(flat, width)
            step = min(256, units)
            for first in range(0, units, step):
                gate = jnp.dot(
                    inputs, gate_v[:, first : first + step], preferred_element_type=jnp.float32
                )
                up = jnp.dot(
                    inputs, up_v[:, first : first + step], preferred_element_type=jnp.float32
                )
                hidden[:, first : first + step] = clamped_unit(gate, up).astype(jnp.bfloat16)
            for first in range(0, width, 256):
                piece = jnp.dot(
                    hidden[...], down_v[:, first : first + 256], preferred_element_type=jnp.float32
                )
                parts[k, :, :, first : first + 256] = piece.astype(jnp.bfloat16).reshape(
                    4, cap, 256
                )
            pair_copy(k).start()
            part_copy(k).start()

        @pl.when(k == n // 4)
        def _():
            for z in range(n // 2):
                if z:
                    kv_z_copy(z).wait_recv()
                kv_y_copy(z).start()

        @pl.when(k == n // 4 + 1)
        def _():
            for z in range(n // 2):
                kv_y_copy(z).wait_recv()

        for turn in range(4):

            @pl.when(k == n // 4 + 1 + turn)
            def _():
                for head in range(turn, local_heads, 4):
                    attend(head)

        @pl.when(k == n // 4 + 5)
        def _():
            for first in range(0, width, 256):
                piece = jnp.dot(
                    heads[...], out_v[:, first : first + 256], preferred_element_type=jnp.float32
                )
                shares[:, :, first : first + 256] = piece.astype(jnp.bfloat16).reshape(
                    4, tokens // 4, 256
                )
            for shift in range(1, 4):
                mix_copy(shift).start()

    ret[me] = final[0]
    total = shares[tp].astype(jnp.float32)
    for shift in range(1, 4):
        mix_copy(shift).wait_recv()
        total = total + landed[shift - 1].astype(jnp.float32)
    mixer_out[...] = total.astype(jnp.bfloat16)
    for shift in range(1, 4):
        mix_copy(shift).wait_send()
    for z in range(n // 2):
        if z:
            kv_z_copy(z).wait_send()
        kv_y_copy(z).wait_send()

    @pl.loop(0, n)
    def _(k):
        for made in (core_copy, across_copy, core_across_copy, part_copy, pair_copy, sums_copy):
            made(k).wait_send()

        @pl.when(k >= 1)
        def _():
            out_copy(k).wait_send()
            back_copy(k).wait_send()
            back_copy(k).wait_recv()


def run_exchange(
    n, outgoing, kv, queries_a, queries_b, head_gain, lambdas, w_gate, w_up, w_down, w_out
):
    _, cap, width = outgoing.shape
    units = w_gate.shape[1]
    block = (n, cap, width)
    vmem = pl.BlockSpec(memory_space=pltpu.VMEM)
    hbm = pl.BlockSpec(memory_space=pl.ANY)
    return pl.pallas_call(
        functools.partial(exchange, n),
        out_shape=(
            jax.ShapeDtypeStruct(block, jnp.bfloat16),
            jax.ShapeDtypeStruct((kv.shape[0] // 4, width), jnp.bfloat16),
        ),
        in_specs=[vmem] * 5 + [pl.BlockSpec(memory_space=pltpu.SMEM)] + [hbm] * 4,
        out_specs=(vmem, vmem),
        scratch_shapes=[
            pltpu.VMEM((n, 4, cap, width), jnp.bfloat16),
            pltpu.VMEM((n, 4, cap, width), jnp.bfloat16),
            pltpu.VMEM(block, jnp.bfloat16),
            pltpu.VMEM(block, jnp.bfloat16),
            pltpu.VMEM(block, jnp.bfloat16),
            pltpu.VMEM(block, jnp.bfloat16),
            pltpu.VMEM(block, jnp.bfloat16),
            pltpu.VMEM((4 * cap, units), jnp.bfloat16),
            pltpu.VMEM(w_gate.shape, jnp.bfloat16),
            pltpu.VMEM(w_up.shape, jnp.bfloat16),
            pltpu.VMEM(w_down.shape, jnp.bfloat16),
            pltpu.VMEM(w_out.shape, jnp.bfloat16),
            pltpu.VMEM((n,) + kv.shape, jnp.bfloat16),
            pltpu.VMEM((kv.shape[0], w_out.shape[0]), jnp.bfloat16),
            pltpu.VMEM((4, kv.shape[0] // 4, width), jnp.bfloat16),
            pltpu.VMEM((3, kv.shape[0] // 4, width), jnp.bfloat16),
            pltpu.SemaphoreType.DMA((11, n)),
            pltpu.SemaphoreType.DMA((11, n)),
            pltpu.SemaphoreType.DMA((6,)),
        ],
        compiler_params=pltpu.CompilerParams(
            collective_id=0, has_side_effects=True, vmem_limit_bytes=60 * 2**20
        ),
        name="exchange",
    )(
        outgoing, kv, queries_a, queries_b, head_gain.reshape(1, -1), lambdas,
        w_gate, w_up, w_down, w_out,
    )


def fast_body(
    queries_a, queries_b, keys_a, keys_b, values, lambdas, head_gain, w_out,
    moe_tokens, moe_gain, routes, route_weights, w_gate, w_up, w_down,
):
    n = lax.axis_size("ep")
    tok_rows, width = moe_tokens.shape
    cap = 3 * tok_rows * TOP // (2 * n)
    inputs = moe_tokens.astype(jnp.float32)
    normed = (
        inputs * lax.rsqrt(jnp.mean(inputs * inputs, axis=-1, keepdims=True) + eps) * moe_gain
    ).astype(jnp.bfloat16)
    named = routes[:, :, None] == jnp.arange(n, dtype=jnp.int32)[None, None, :]
    member = jnp.any(named, axis=1)
    earlier = jnp.tril(jnp.ones((tok_rows, tok_rows), jnp.bfloat16), -1)
    place = jnp.dot(
        earlier, member.astype(jnp.bfloat16), preferred_element_type=jnp.float32
    ).astype(jnp.int32)
    slot = jnp.where(member, place, cap).T
    pick = (slot[:, None, :] == jnp.arange(cap, dtype=jnp.int32)[None, :, None]).reshape(
        n * cap, tok_rows
    )
    outgoing = (
        jnp.dot(pick.astype(jnp.bfloat16), normed, preferred_element_type=jnp.float32)
        .astype(jnp.bfloat16)
        .reshape(n, cap, width)
    )
    kv = jnp.concatenate([keys_a, keys_b, values], axis=1)
    returned, mixer_out = run_exchange(
        n, outgoing, kv, queries_a, queries_b, head_gain, lambdas,
        w_gate[0], w_up[0], w_down[0], w_out,
    )
    slot_ids = routes * cap + jnp.sum(jnp.where(named, place[:, None, :], 0), axis=2)
    table = returned.reshape(n * cap, width)
    total = 0.0
    for k in range(TOP):
        chosen = slot_ids[:, k : k + 1] == jnp.arange(n * cap, dtype=jnp.int32)[None, :]
        total = total + route_weights[:, k : k + 1] * jnp.dot(
            chosen.astype(jnp.bfloat16), table, preferred_element_type=jnp.float32
        )
    return (mixer_out, total.astype(jnp.bfloat16))


def whole_body(*args):
    n, n_tp = lax.axis_size("ep"), lax.axis_size("tp")
    tok_rows, w_gate = args[8].shape[0], args[12]
    cap = 3 * tok_rows * TOP // (2 * n)
    if w_gate.shape[0] == 1 and n_tp == 4 and n & (n - 1) == 0 and n >= 8 and cap % 16 == 0:
        return fast_body(*args)
    return body(*args)


def solution(mesh):
    return jax.shard_map(
        whole_body,
        mesh=mesh,
        in_specs=(
            P("ep", "tp"),
            P("ep", "tp"),
            P("ep", "tp"),
            P("ep", "tp"),
            P("ep", "tp"),
            P("tp"),
            P(),
            P("tp", None),
            P(("ep", "tp"), None),
            P(),
            P(("ep", "tp"), None),
            P(("ep", "tp"), None),
            P("ep", None, "tp"),
            P("ep", None, "tp"),
            P("ep", "tp", None),
        ),
        out_specs=(P(("ep", "tp"), None), P(("ep", "tp"), None)),
        check_vma=False,
    )
```
